32 devices in a mesh: sp: 4 (over z), dp: 8 (over y, x, core).
Axes of the slice: x: 2, y: 2, z: 4, core: 2. Of those that a mesh axis runs over, the one named last changes fastest.
Arguments:
- up_pre: bfloat16 [8, 1536, 2048], P('dp', 'sp'), may hold values from -6 to 6
- mix_pre: bfloat16 [8, 1536, 2048], P('dp', 'sp'), may hold values from -6 to 6
- ln_gain: float32 [2048], replicated, may hold values from 0.1 to 1.9
- mix_weight: bfloat16 [16, 128, 128], replicated, may hold values from -0.5 to 0.5
- mix_bias: float32 [16, 128], replicated, may hold values from 0.1 to 1.9
- out_weight: bfloat16 [2048, 2048], P('sp', 'dp'), may hold values from -0.125 to 0.125
Outputs:
- mixed_out: bfloat16 [8, 1536, 2048], P('dp', 'sp')
The draws below stay inside these ranges and needn't reach their ends.
All inputs are finite; a program needn't handle non-finite values.
Results may differ from the reference program's by a relative error of at most 0.012.
Values may be sent and summed in bfloat16 or wider, within the bound.
A program may use at most 64 MiB of HBM per device.

```python
import jax
import jax.numpy as jnp
from jax import lax

D = 2048
E = 2048
GROUPS = 16
BLOCK = 128
SEQS = 8
LENGTH = 1536


def level_of(key, extent, cuts, least, top_value):
    def one(dim, blocks):
        heights = jax.random.uniform(jax.random.fold_in(jax.random.fold_in(key, 6), dim), (blocks,), jnp.float32, least / len(cuts), top_value / len(cuts))
        return jnp.repeat(jnp.exp(heights), extent[dim] // blocks).reshape((-1,) + (1,) * (len(extent) - dim - 1))

    factor_of = one(*cuts[0])
    for cut in cuts[1:]:
        factor_of = factor_of * one(*cut)
    return factor_of


def noise(own_key, extent, scale, reach, cuts=(), kind=jnp.bfloat16):
    loudness = level_of(own_key, extent, cuts, -0.22, 0.18) if cuts else 1.0
    entries = jax.random.normal(own_key, extent, jnp.float32) * scale * loudness
    return jnp.minimum(jnp.maximum(entries, -reach), reach).astype(kind)


def setup_inputs(seed: int = 0) -> dict:
    seeds = jax.random.split(jax.random.key(seed), 7)
    return {
        "up_pre": noise(seeds[0], (SEQS, LENGTH, E), 1.0, 6.0, ((0, 8), (1, 4))),
        "mix_pre": noise(seeds[1], (SEQS, LENGTH, E), 1.0, 6.0, ((0, 8), (1, 4))),
        "ln_gain": jnp.clip(1.0 + 0.18 * jax.random.normal(seeds[2], (E,), jnp.float32), 0.1, 1.9),
        "mix_weight": noise(seeds[3], (GROUPS, BLOCK, BLOCK), BLOCK ** -0.5, 0.5),
        "mix_bias": jnp.clip(1.0 + 0.18 * jax.random.normal(seeds[4], (GROUPS, BLOCK), jnp.float32), 0.1, 1.9),
        "out_weight": noise(seeds[5], (E, D), E ** -0.5, 0.125, ((0, 4), (1, 8))),
    }


norm_epsilon = 1e-05

def one_sequence(operands):
    up_seq, mix_seq, ln_gain, masked, mix_bias, out_weight = operands
    up_act = jax.nn.gelu(up_seq.astype(jnp.float32), approximate=False).astype(jnp.bfloat16)
    activated = jax.nn.gelu(mix_seq.astype(jnp.float32), approximate=False)
    center = lax.optimization_barrier(jnp.mean(activated, axis=-1, keepdims=True))
    spread = lax.optimization_barrier(jnp.mean(jnp.square(activated - center), axis=-1, keepdims=True))
    normed = ((activated - center) * lax.rsqrt(spread + norm_epsilon) * ln_gain).astype(jnp.bfloat16)
    row_count, channels = normed.shape
    blocks = normed.astype(jnp.float32).reshape(row_count // BLOCK, BLOCK, GROUPS, channels // GROUPS)
    mixed_sum = jnp.einsum('gts,nsgc->ntgc', masked, blocks)
    mixed_sum = mixed_sum + jnp.transpose(mix_bias)[None, :, :, None]
    gated = (up_act.astype(jnp.float32) * mixed_sum.reshape(row_count, channels)).astype(jnp.bfloat16)
    return jnp.dot(gated, out_weight, preferred_element_type=jnp.float32).astype(jnp.bfloat16)

def reference(up_pre, mix_pre, ln_gain, mix_weight, mix_bias, out_weight):
    positions = jnp.arange(BLOCK, dtype=jnp.int32)
    causal = positions[:, None] >= positions[None, :]
    masked = jnp.where(causal[None], mix_weight.astype(jnp.float32), jnp.float32(0.0))

    def apply_one(pair):
        return one_sequence((pair[0], pair[1], ln_gain, masked, mix_bias, out_weight))
    return lax.map(apply_one, (up_pre, mix_pre))
```

```python
import functools

import jax
import jax.numpy as jnp
from jax import lax
from jax.experimental import pallas as pl
from jax.experimental.pallas import tpu as pltpu
from jax.sharding import PartitionSpec as P

BLOCK = 128
LANES = 128
CHUNK = 16
MESH = pl.DeviceIdType.MESH

norm_epsilon = 1e-05


def gelu(values):
    return 0.5 * values * (1.0 + lax.erf(values * 0.7071067811865476))


def slot_list(depth):
    slots = [("own", 0)]
    for hop in range(1, depth):
        slots += [("up", hop), ("down", hop)]
    return slots


def kernel(
    depth, rows_c,
    up_hbm, mix_hbm, gain_ref, weight_hbm, bias_ref, shard_hbm,
    out_ref,
    held, up_buf, mix_buf, weight_buf, masked, bias_full, normed, up_act, gated, total,
    in_sem, send_sem, recv_sem,
):
    rows, channels = up_hbm.shape
    groups = weight_hbm.shape[0]
    width = channels // groups
    block_count = rows // BLOCK
    shard_rows, shard_cols = shard_hbm.shape
    chips = held.shape[1]
    rows_ab = shard_rows - rows_c
    rows_a = rows_ab // 32 * 16

    z = lax.axis_index("sp")
    d = lax.axis_index("dp")
    core = lax.rem(d, 2)
    chip = d // 2
    x = lax.rem(chip, 2)
    y = chip // 2
    chip_x = chip + 1 - 2 * x
    chip_y = chip + 2 - 4 * y
    chip_xy = chip_x + 2 - 4 * y
    to_x = {"dp": chip_x * 2 + core}
    to_y = {"dp": chip_y * 2 + core}
    partner = {"dp": chip * 2 + 1 - core}
    above = {"sp": z + 1}
    below = {"sp": z - 1}
    has_above = z < depth - 1
    has_below = z > 0

    def held_at(cc, q, origin, part):
        start, count = {
            "a": (0, rows_a),
            "b": (rows_a, rows_ab - rows_a),
            "ab": (0, rows_ab),
            "c": (rows_ab, rows_c),
            "all": (0, shard_rows),
        }[part]
        place = pl.ds(pl.multiple_of(origin * shard_rows + start, 16), count)
        return held.at[cc, q, place, :]

    names = {}

    def index(name):
        return names.setdefault(name, len(names))

    def copy(ref, name, target):
        k = index(name)
        return pltpu.make_async_remote_copy(
            src_ref=ref, dst_ref=ref, send_sem=send_sem.at[k], recv_sem=recv_sem.at[k],
            device_id=target, device_id_type=MESH,
        )

    slots = slot_list(depth)

    def origin_of(n):
        way, hop = slots[n]
        return z if way == "own" else z - hop if way == "up" else z + hop

    def when(n, body):
        way, hop = slots[n]
        if way == "own":
            body()
        elif way == "up":
            pl.when(z >= hop)(body)
        else:
            pl.when(z <= depth - 1 - hop)(body)

    def sends(n):
        way, hop = slots[n]
        o = origin_of(n)
        if way in ("own", "up") and hop + 1 < depth:
            @pl.when(has_above)
            def _():
                copy(held_at(core, chip, o, "ab"), ("z", "up", hop + 1), above).start()
        if way in ("own", "down") and hop + 1 < depth:
            @pl.when(has_below)
            def _():
                copy(held_at(core, chip, o, "ab"), ("z", "down", hop + 1), below).start()
        copy(held_at(core, chip, o, "a"), ("xa", n), to_x).start()
        copy(held_at(core, chip, o, "b"), ("yb", n), to_y).start()
        copy(held_at(core, chip, o, "b"), ("xb", n), to_x).start()
        copy(held_at(core, chip, o, "a"), ("ya", n), to_y).start()

    def recv_z(n):
        def body():
            way, hop = slots[n]
            copy(held_at(core, chip, origin_of(n), "ab"), ("z", way, hop), above).wait_recv()
            sends(n)
        when(n, body)

    def turn(n):
        def body():
            o = origin_of(n)
            copy(held_at(core, chip_x, o, "a"), ("xa", n), to_x).wait_recv()
            copy(held_at(core, chip_x, o, "a"), ("ya2", n), to_y).start()
            copy(held_at(core, chip_y, o, "b"), ("yb", n), to_y).wait_recv()
            copy(held_at(core, chip_y, o, "b"), ("xb2", n), to_x).start()
        when(n, body)

    def finish(n):
        def body():
            o = origin_of(n)
            copy(held_at(core, chip_x, o, "b"), ("xb", n), to_x).wait_recv()
            copy(held_at(core, chip_y, o, "a"), ("ya", n), to_y).wait_recv()
            copy(held_at(core, chip_xy, o, "b"), ("xb2", n), to_x).wait_recv()
            copy(held_at(core, chip_xy, o, "a"), ("ya2", n), to_y).wait_recv()
            copy(held_at(core, slice(None), o, "ab"), ("p", n), partner).start()
        when(n, body)

    def recv_partner(n):
        def body():
            o = origin_of(n)
            copy(held_at(1 - core, slice(None), o, "ab"), ("p", n), partner).wait_recv()
            if rows_c:
                copy(held_at(1 - core, slice(None), o, "c"), ("pc", n), partner).wait_recv()
        when(n, body)

    def c_pass(n):
        way, hop = slots[n]
        o = origin_of(n)
        if way in ("own", "up") and hop + 1 < depth:
            @pl.when(has_above)
            def _():
                copy(held_at(core, slice(None), o, "c"), ("zc", "up", hop + 1), above).start()
        if way in ("own", "down") and hop + 1 < depth:
            @pl.when(has_below)
            def _():
                copy(held_at(core, slice(None), o, "c"), ("zc", "down", hop + 1), below).start()
        copy(held_at(core, slice(None), o, "c"), ("pc", n), partner).start()

    def c_start():
        if rows_c:
            copy(held_at(core, chip, z, "c"), ("cx",), to_x).start()
            copy(held_at(core, chip, z, "c"), ("cy",), to_y).start()

    def c_turn():
        if rows_c:
            copy(held_at(core, chip_x, z, "c"), ("cx",), to_x).wait_recv()
            copy(held_at(core, chip_x, z, "c"), ("cy2",), to_y).start()

    def c_layer():
        if rows_c:
            copy(held_at(core, chip_y, z, "c"), ("cy",), to_y).wait_recv()
            copy(held_at(core, chip_xy, z, "c"), ("cy2",), to_y).wait_recv()
            c_pass(0)

    def c_recv(n):
        if rows_c:
            def body():
                way, hop = slots[n]
                copy(held_at(core, slice(None), origin_of(n), "c"), ("zc", way, hop), above).wait_recv()
                c_pass(n)
            when(n, body)

    own = pltpu.make_async_copy(shard_hbm, held_at(core, chip, z, "all"), in_sem.at[0])
    own.start()
    loads = []
    for b in range(block_count):
        place = pl.ds(b * BLOCK, BLOCK)
        loads.append((
            pltpu.make_async_copy(mix_hbm.at[place], mix_buf.at[place], in_sem.at[2 + 2 * b]),
            pltpu.make_async_copy(up_hbm.at[place], up_buf.at[place], in_sem.at[3 + 2 * b]),
        ))
        loads[-1][0].start()
        loads[-1][1].start()
    weights = pltpu.make_async_copy(weight_hbm, weight_buf, in_sem.at[1])
    weights.start()

    barrier = pltpu.get_barrier_semaphore()
    for target in (to_x, to_y, partner):
        pl.semaphore_signal(barrier, inc=1, device_id=target, device_id_type=MESH)

    @pl.when(has_above)
    def _():
        pl.semaphore_signal(barrier, inc=1, device_id=above, device_id_type=MESH)

    @pl.when(has_below)
    def _():
        pl.semaphore_signal(barrier, inc=1, device_id=below, device_id_type=MESH)

    pl.semaphore_wait(barrier, 3 + has_above.astype(jnp.int32) + has_below.astype(jnp.int32))

    own.wait()
    sends(0)
    c_start()

    def prepare():
        weights.wait()
        positions = lax.broadcasted_iota(jnp.int32, (BLOCK, BLOCK), 0)
        sources = lax.broadcasted_iota(jnp.int32, (BLOCK, BLOCK), 1)

        def one(g, carry):
            kept = weight_buf[g].astype(jnp.float32)
            masked[g] = jnp.where(positions >= sources, kept, 0.0).astype(jnp.bfloat16)
            bias_full[g] = jnp.broadcast_to(bias_ref[pl.ds(g, 1), :], (BLOCK, BLOCK)).T
            return carry

        lax.fori_loop(0, groups, one, 0)

    def activate(b, first, last):
        def one(i, carry):
            place = pl.ds(pl.multiple_of(i * CHUNK, CHUNK), CHUNK)
            source = pl.ds(pl.multiple_of(b * BLOCK + i * CHUNK, CHUNK), CHUNK)
            activated = gelu(mix_buf[source, :].astype(jnp.float32))
            center = jnp.sum(activated, axis=-1, keepdims=True) * (1.0 / channels)
            activated = activated - center
            spread = jnp.sum(activated * activated, axis=-1, keepdims=True) * (1.0 / channels)
            scale = lax.rsqrt(spread + norm_epsilon)
            normed[place, :] = (activated * scale * gain_ref[...]).astype(jnp.bfloat16)
            up_act[place, :] = gelu(up_buf[source, :].astype(jnp.float32)).astype(jnp.bfloat16)
            return carry

        lax.fori_loop(first, last, one, 0)

    def mix(b):
        def one(g, carry):
            cols = pl.ds(pl.multiple_of(g * width, LANES), width)
            mixed = jnp.dot(masked[g], normed[:, cols], preferred_element_type=jnp.float32)
            spread_bias = jnp.concatenate([bias_full[g]] * (width // BLOCK), axis=1)
            gated[pl.ds(b * BLOCK, BLOCK), cols] = (
                up_act[:, cols].astype(jnp.float32) * (mixed + spread_bias)
            ).astype(jnp.bfloat16)
            return carry

        lax.fori_loop(0, groups, one, 0)

    def project(n):
        def body():
            o = origin_of(n)
            left = gated[:, pl.ds(pl.multiple_of(o * shard_rows, LANES), shard_rows)]
            depth_rows = pl.ds(pl.multiple_of(o * shard_rows, 16), shard_rows)

            def one(j, carry):
                cols = pl.ds(pl.multiple_of(j * shard_cols, LANES), shard_cols)
                term = jnp.dot(
                    left, held[lax.rem(j, 2), j // 2, depth_rows, :],
                    preferred_element_type=jnp.float32,
                )
                if n == 0:
                    total[:, cols] = term
                else:
                    total[:, cols] += term
                return carry

            lax.fori_loop(0, 2 * chips, one, 0)
        when(n, body)

    per_block = BLOCK // CHUNK
    half = per_block // 2

    events = [[lambda: turn(0)]]
    for hop in range(1, depth):
        up, down = 2 * hop - 1, 2 * hop
        group = [functools.partial(recv_z, up), functools.partial(recv_z, down)]
        events.append(group)
        if hop == 1:
            events.append([c_turn])
        events.append([functools.partial(turn, up), functools.partial(turn, down)])
        if hop == 1:
            events.append([c_layer])
        if hop > 1:
            events.append([functools.partial(c_recv, up - 2), functools.partial(c_recv, down - 2)])
    work = [prepare]
    for b in range(block_count):
        def load(b=b):
            loads[b][0].wait()
            loads[b][1].wait()
            activate(b, 0, half)
        work += [load, functools.partial(activate, b, half, per_block), functools.partial(mix, b)]
    while events or work:
        for _ in range(2 if len(work) > 8 else 1):
            if work:
                work.pop(0)()
        if events:
            for event in events.pop(0):
                event()

    last = len(slots) - 2
    finish(0)
    finish(1)
    finish(2)
    recv_partner(0)
    project(0)
    for n in range(3, len(slots)):
        finish(n)
    c_recv(last)
    c_recv(last + 1)
    for n in range(1, len(slots)):
        recv_partner(n)
        project(n)
    out_ref[...] = total[...].astype(out_ref.dtype)

    for n in range(len(slots)):
        way, hop = slots[n]

        def body():
            o = origin_of(n)
            for name, part in (("xa", "a"), ("yb", "b"), ("xb", "b"), ("ya", "a"), ("ya2", "a"), ("xb2", "b")):
                copy(held_at(core, chip, o, part), (name, n), to_x).wait_send()
            copy(held_at(core, slice(None), o, "ab"), ("p", n), partner).wait_send()
            if rows_c:
                copy(held_at(core, slice(None), o, "c"), ("pc", n), partner).wait_send()
            for direction, cond, target in (("up", has_above, above), ("down", has_below, below)):
                if way in ("own", direction) and hop + 1 < depth:
                    @pl.when(cond)
                    def _():
                        copy(held_at(core, chip, o, "ab"), ("z", direction, hop + 1), target).wait_send()
                        if rows_c:
                            copy(held_at(core, slice(None), o, "c"), ("zc", direction, hop + 1), target).wait_send()
        when(n, body)
    if rows_c:
        for name in ("cx", "cy", "cy2"):
            copy(held_at(core, chip, z, "c"), (name,), to_x).wait_send()


def semaphores(depth):
    return 10 * (2 * depth - 1) + 3


def fused(depth, columns, up_rows, mix_rows, ln_gain, mix_weight, mix_bias, out_weight):
    rows, channels = up_rows.shape
    groups = mix_weight.shape[0]
    shard_rows, shard_cols = out_weight.shape
    chips = columns // 2
    rows_c = shard_rows * 3 // 16 // 32 * 32
    any_space = pl.BlockSpec(memory_space=pl.ANY)
    vmem = pl.BlockSpec(memory_space=pltpu.VMEM)
    return pl.pallas_call(
        functools.partial(kernel, depth, rows_c),
        out_shape=jax.ShapeDtypeStruct((rows, shard_cols * columns), jnp.bfloat16),
        in_specs=[any_space, any_space, vmem, any_space, vmem, any_space],
        out_specs=vmem,
        scratch_shapes=[
            pltpu.VMEM((2, chips, depth * shard_rows, shard_cols), jnp.bfloat16),
            pltpu.VMEM((rows, channels), jnp.bfloat16),
            pltpu.VMEM((rows, channels), jnp.bfloat16),
            pltpu.VMEM((groups, BLOCK, BLOCK), jnp.bfloat16),
            pltpu.VMEM((groups, BLOCK, BLOCK), jnp.bfloat16),
            pltpu.VMEM((groups, BLOCK, BLOCK), jnp.float32),
            pltpu.VMEM((BLOCK, channels), jnp.bfloat16),
            pltpu.VMEM((BLOCK, channels), jnp.bfloat16),
            pltpu.VMEM((rows, channels), jnp.bfloat16),
            pltpu.VMEM((rows, shard_cols * columns), jnp.float32),
            pltpu.SemaphoreType.DMA((2 + 2 * (rows // BLOCK),)),
            pltpu.SemaphoreType.DMA((semaphores(depth),)),
            pltpu.SemaphoreType.DMA((semaphores(depth),)),
        ],
        compiler_params=pltpu.CompilerParams(
            collective_id=0, has_side_effects=True, vmem_limit_bytes=60 * 2**20
        ),
    )(up_rows, mix_rows, ln_gain[None], mix_weight, mix_bias, out_weight)


def plain(up_rows, mix_rows, ln_gain, mix_weight, mix_bias, out_weight):
    up_act = gelu(up_rows.astype(jnp.float32)).astype(jnp.bfloat16)
    activated = gelu(mix_rows.astype(jnp.float32))
    center = jnp.mean(activated, axis=-1, keepdims=True)
    spread = jnp.mean(jnp.square(activated - center), axis=-1, keepdims=True)
    normed = ((activated - center) * lax.rsqrt(spread + norm_epsilon) * ln_gain).astype(
        jnp.bfloat16
    )
    positions = lax.broadcasted_iota(jnp.int32, (BLOCK, BLOCK), 0)
    sources = lax.broadcasted_iota(jnp.int32, (BLOCK, BLOCK), 1)
    masked = jnp.where((positions >= sources)[None], mix_weight, jnp.zeros_like(mix_weight))
    row_count, channels = normed.shape
    groups = masked.shape[0]
    blocks = normed.reshape(row_count // BLOCK, BLOCK, groups, channels // groups)
    mixed = jnp.einsum("gts,nsgc->ntgc", masked, blocks, preferred_element_type=jnp.float32)
    mixed = mixed + jnp.transpose(mix_bias)[None, :, :, None]
    gated = (up_act.astype(jnp.float32) * mixed.reshape(row_count, channels)).astype(jnp.bfloat16)
    rows_whole = lax.all_gather(out_weight, "sp", axis=0, tiled=True)
    whole = lax.all_gather(rows_whole, "dp", axis=1, tiled=True)
    return jnp.dot(gated, whole, preferred_element_type=jnp.float32).astype(jnp.bfloat16)


def solution(mesh):
    depth, columns = mesh.shape["sp"], mesh.shape["dp"]

    def per_device(up_pre, mix_pre, ln_gain, mix_weight, mix_bias, out_weight):
        shard_rows, shard_cols = out_weight.shape
        fits = (
            columns == 8
            and depth > 1
            and up_pre.shape[0] == 1
            and shard_cols % LANES == 0
            and shard_rows % LANES == 0
            and up_pre.shape[1] % BLOCK == 0
            and up_pre.shape[2] % (mix_weight.shape[0] * LANES) == 0
        )
        form = functools.partial(fused, depth, columns) if fits else plain
        return form(up_pre[0], mix_pre[0], ln_gain, mix_weight, mix_bias, out_weight)[None]

    return jax.shard_map(
        per_device,
        mesh=mesh,
        in_specs=(P("dp", "sp", None), P("dp", "sp", None), P(), P(), P(), P("sp", "dp")),
        out_specs=P("dp", "sp", None),
        check_vma=False,
    )
```

```python
import functools

import jax
import jax.numpy as jnp
from jax import lax
from jax.experimental import pallas as pl
from jax.experimental.pallas import tpu as pltpu
from jax.sharding import PartitionSpec as P

BLOCK = 128
LANES = 128
CHUNK = 16
MESH = pl.DeviceIdType.MESH

norm_epsilon = 1e-05


def gelu(values):
    return 0.5 * values * (1.0 + lax.erf(values * 0.7071067811865476))


def slot_list(depth):
    slots = [("own", 0)]
    for hop in range(1, depth):
        slots += [("up", hop), ("down", hop)]
    return slots


def kernel(
    depth, rows_c,
    up_hbm, mix_hbm, gain_hbm, weight_hbm, bias_hbm, shard_hbm,
    out_ref,
    held, gain_ref, bias_ref, up_buf, mix_buf, weight_buf, masked, bias_full, normed, up_act, gated, total,
    in_sem, send_sem, recv_sem,
):
    rows, channels = up_hbm.shape
    groups = weight_hbm.shape[0]
    width = channels // groups
    block_count = rows // BLOCK
    shard_rows, shard_cols = shard_hbm.shape
    chips = held.shape[1]
    rows_ab = shard_rows - rows_c
    rows_a = rows_ab // 32 * 16

    z = lax.axis_index("sp")
    d = lax.axis_index("dp")
    core = lax.rem(d, 2)
    chip = d // 2
    x = lax.rem(chip, 2)
    y = chip // 2
    chip_x = chip + 1 - 2 * x
    chip_y = chip + 2 - 4 * y
    chip_xy = chip_x + 2 - 4 * y
    to_x = {"dp": chip_x * 2 + core}
    to_y = {"dp": chip_y * 2 + core}
    partner = {"dp": chip * 2 + 1 - core}
    above = {"sp": z + 1}
    below = {"sp": z - 1}
    has_above = z < depth - 1
    has_below = z > 0

    def held_at(cc, q, origin, part):
        start, count = {
            "a": (0, rows_a),
            "b": (rows_a, rows_ab - rows_a),
            "ab": (0, rows_ab),
            "c": (rows_ab, rows_c),
            "all": (0, shard_rows),
        }[part]
        place = pl.ds(pl.multiple_of(origin * shard_rows + start, 16), count)
        return held.at[cc, q, place, :]

    names = {}

    def index(name):
        return names.setdefault(name, len(names))

    def copy(ref, name, target):
        k = index(name)
        return pltpu.make_async_remote_copy(
            src_ref=ref, dst_ref=ref, send_sem=send_sem.at[k], recv_sem=recv_sem.at[k],
            device_id=target, device_id_type=MESH,
        )

    slots = slot_list(depth)

    def origin_of(n):
        way, hop = slots[n]
        return z if way == "own" else z - hop if way == "up" else z + hop

    def when(n, body):
        way, hop = slots[n]
        if way == "own":
            body()
        elif way == "up":
            pl.when(z >= hop)(body)
        else:
            pl.when(z <= depth - 1 - hop)(body)

    def sends(n):
        way, hop = slots[n]
        o = origin_of(n)
        if way in ("own", "up") and hop + 1 < depth:
            @pl.when(has_above)
            def _():
                copy(held_at(core, chip, o, "ab"), ("z", "up", hop + 1), above).start()
        if way in ("own", "down") and hop + 1 < depth:
            @pl.when(has_below)
            def _():
                copy(held_at(core, chip, o, "ab"), ("z", "down", hop + 1), below).start()
        copy(held_at(core, chip, o, "a"), ("xa", n), to_x).start()
        copy(held_at(core, chip, o, "b"), ("yb", n), to_y).start()
        copy(held_at(core, chip, o, "b"), ("xb", n), to_x).start()
        copy(held_at(core, chip, o, "a"), ("ya", n), to_y).start()
        copy(held_at(core, chip, o, "ab"), ("p", 0, n), partner).start()

    def recv_z(n):
        def body():
            way, hop = slots[n]
            copy(held_at(core, chip, origin_of(n), "ab"), ("z", way, hop), above).wait_recv()
            sends(n)
        when(n, body)

    def turn(n):
        def body():
            o = origin_of(n)
            copy(held_at(core, chip_x, o, "a"), ("xa", n), to_x).wait_recv()
            copy(held_at(core, chip_x, o, "a"), ("ya2", n), to_y).start()
            copy(held_at(core, chip_y, o, "b"), ("yb", n), to_y).wait_recv()
            copy(held_at(core, chip_y, o, "b"), ("xb2", n), to_x).start()
        when(n, body)

    def finish(n):
        def body():
            o = origin_of(n)
            copy(held_at(core, chip_x, o, "b"), ("xb", n), to_x).wait_recv()
            copy(held_at(core, chip_x, o, "ab"), ("p", 1, n), partner).start()
            copy(held_at(core, chip_y, o, "a"), ("ya", n), to_y).wait_recv()
            copy(held_at(core, chip_y, o, "ab"), ("p", 2, n), partner).start()
            copy(held_at(core, chip_xy, o, "b"), ("xb2", n), to_x).wait_recv()
            copy(held_at(core, chip_xy, o, "a"), ("ya2", n), to_y).wait_recv()
            copy(held_at(core, chip_xy, o, "ab"), ("p", 3, n), partner).start()
        when(n, body)

    def recv_partner(n):
        def body():
            o = origin_of(n)
            for k, q in enumerate((chip, chip_x, chip_y, chip_xy)):
                copy(held_at(1 - core, q, o, "ab"), ("p", k, n), partner).wait_recv()
            if rows_c:
                copy(held_at(1 - core, slice(None), o, "c"), ("pc", n), partner).wait_recv()
        when(n, body)

    def c_pass(n):
        way, hop = slots[n]
        o = origin_of(n)
        if way in ("own", "up") and hop + 1 < depth:
            @pl.when(has_above)
            def _():
                copy(held_at(core, slice(None), o, "c"), ("zc", "up", hop + 1), above).start()
        if way in ("own", "down") and hop + 1 < depth:
            @pl.when(has_below)
            def _():
                copy(held_at(core, slice(None), o, "c"), ("zc", "down", hop + 1), below).start()
        copy(held_at(core, slice(None), o, "c"), ("pc", n), partner).start()

    def c_start():
        if rows_c:
            copy(held_at(core, chip, z, "c"), ("cx",), to_x).start()
            copy(held_at(core, chip, z, "c"), ("cy",), to_y).start()

    def c_turn():
        if rows_c:
            copy(held_at(core, chip_x, z, "c"), ("cx",), to_x).wait_recv()
            copy(held_at(core, chip_x, z, "c"), ("cy2",), to_y).start()

    def c_layer():
        if rows_c:
            copy(held_at(core, chip_y, z, "c"), ("cy",), to_y).wait_recv()
            copy(held_at(core, chip_xy, z, "c"), ("cy2",), to_y).wait_recv()
            c_pass(0)

    def c_recv(n):
        if rows_c:
            def body():
                way, hop = slots[n]
                copy(held_at(core, slice(None), origin_of(n), "c"), ("zc", way, hop), above).wait_recv()
                c_pass(n)
            when(n, body)

    own = pltpu.make_async_copy(shard_hbm, held_at(core, chip, z, "all"), in_sem.at[0])
    own.start()
    weights = pltpu.make_async_copy(weight_hbm, weight_buf, in_sem.at[1])
    gain = pltpu.make_async_copy(gain_hbm, gain_ref, in_sem.at[2 + 2 * block_count])
    bias = pltpu.make_async_copy(bias_hbm, bias_ref, in_sem.at[3 + 2 * block_count])
    for part in (weights, gain, bias):
        part.start()
    loads = []
    for b in range(block_count):
        place = pl.ds(b * BLOCK, BLOCK)
        loads.append((
            pltpu.make_async_copy(mix_hbm.at[place], mix_buf.at[place], in_sem.at[2 + 2 * b]),
            pltpu.make_async_copy(up_hbm.at[place], up_buf.at[place], in_sem.at[3 + 2 * b]),
        ))
        loads[-1][0].start()
        loads[-1][1].start()

    barrier = pltpu.get_barrier_semaphore()
    for target in (to_x, to_y, partner):
        pl.semaphore_signal(barrier, inc=1, device_id=target, device_id_type=MESH)

    @pl.when(has_above)
    def _():
        pl.semaphore_signal(barrier, inc=1, device_id=above, device_id_type=MESH)

    @pl.when(has_below)
    def _():
        pl.semaphore_signal(barrier, inc=1, device_id=below, device_id_type=MESH)

    pl.semaphore_wait(barrier, 3 + has_above.astype(jnp.int32) + has_below.astype(jnp.int32))

    own.wait()
    c_start()
    sends(0)

    def prepare():
        weights.wait()
        gain.wait()
        bias.wait()
        positions = lax.broadcasted_iota(jnp.int32, (BLOCK, BLOCK), 0)
        sources = lax.broadcasted_iota(jnp.int32, (BLOCK, BLOCK), 1)

        def one(g, carry):
            kept = weight_buf[g].astype(jnp.float32)
            masked[g] = jnp.where(positions >= sources, kept, 0.0).astype(jnp.bfloat16)
            bias_full[g] = jnp.broadcast_to(bias_ref[pl.ds(g, 1), :], (BLOCK, BLOCK)).T
            return carry

        lax.fori_loop(0, groups, one, 0)

    def activate(b, first, last):
        def one(i, carry):
            place = pl.ds(pl.multiple_of(i * CHUNK, CHUNK), CHUNK)
            source = pl.ds(pl.multiple_of(b * BLOCK + i * CHUNK, CHUNK), CHUNK)
            activated = gelu(mix_buf[source, :].astype(jnp.float32))
            center = jnp.sum(activated, axis=-1, keepdims=True) * (1.0 / channels)
            activated = activated - center
            spread = jnp.sum(activated * activated, axis=-1, keepdims=True) * (1.0 / channels)
            scale = lax.rsqrt(spread + norm_epsilon)
            normed[place, :] = (activated * scale * gain_ref[...]).astype(jnp.bfloat16)
            up_act[place, :] = gelu(up_buf[source, :].astype(jnp.float32)).astype(jnp.bfloat16)
            return carry

        lax.fori_loop(first, last, one, 0, unroll=2)

    def mix(b):
        def one(g, carry):
            cols = pl.ds(pl.multiple_of(g * width, LANES), width)
            mixed = jnp.dot(masked[g], normed[:, cols], preferred_element_type=jnp.float32)
            spread_bias = jnp.concatenate([bias_full[g]] * (width // BLOCK), axis=1)
            gated[pl.ds(b * BLOCK, BLOCK), cols] = (
                up_act[:, cols].astype(jnp.float32) * (mixed + spread_bias)
            ).astype(jnp.bfloat16)
            return carry

        lax.fori_loop(0, groups, one, 0, unroll=8)

    def project(n, cc):
        def body():
            o = origin_of(n)
            left = gated[:, pl.ds(pl.multiple_of(o * shard_rows, LANES), shard_rows)]
            depth_rows = pl.ds(pl.multiple_of(o * shard_rows, 16), shard_rows)

            def one(j, carry):
                cols = pl.ds(pl.multiple_of((2 * j + cc) * shard_cols, LANES), shard_cols)
                term = jnp.dot(
                    left, held[cc, j, depth_rows, :],
                    preferred_element_type=jnp.float32,
                )
                if n == 0:
                    total[:, cols] = term
                else:
                    total[:, cols] += term
                return carry

            lax.fori_loop(0, chips, one, 0, unroll=4)
        when(n, body)

    per_block = BLOCK // CHUNK
    half = per_block // 2

    work = [prepare]
    for b in range(block_count):
        def load(b=b):
            loads[b][0].wait()
            loads[b][1].wait()
            activate(b, 0, half)
        work += [load, functools.partial(activate, b, half, per_block), functools.partial(mix, b)]

    def do(count):
        for step in work[:count]:
            step()
        del work[:count]

    def each(event, hop):
        for n in [0] if hop == 0 else [2 * hop - 1, 2 * hop]:
            event(n)

    def add(hop):
        each(lambda n: project(n, core), hop)
        each(recv_partner, hop)
        each(lambda n: project(n, 1 - core), hop)

    do(3)
    c_turn()
    turn(0)
    do(2)
    each(recv_z, 1)
    do(1)
    c_layer()
    do(2)
    for hop in range(2, depth):
        each(recv_z, hop)
        do(1)
        each(turn, hop - 1)
        do(1)
        each(c_recv, hop - 1)
        each(finish, hop - 2)
        do(len(work))
        if hop > 2:
            add(hop - 3)
    each(turn, depth - 1)
    do(len(work))
    for hop in range(max(0, depth - 3), depth):
        if hop == depth - 1:
            each(c_recv, hop)
        if hop >= max(0, depth - 2):
            each(finish, hop)
        add(hop)
    out_ref[...] = total[...].astype(out_ref.dtype)

    for n in range(len(slots)):
        way, hop = slots[n]

        def body():
            o = origin_of(n)
            for name, part in (("xa", "a"), ("yb", "b"), ("xb", "b"), ("ya", "a"), ("ya2", "a"), ("xb2", "b")):
                copy(held_at(core, chip, o, part), (name, n), to_x).wait_send()
            for k in range(4):
                copy(held_at(core, chip, o, "ab"), ("p", k, n), partner).wait_send()
            if rows_c:
                copy(held_at(core, slice(None), o, "c"), ("pc", n), partner).wait_send()
            for direction, cond, target in (("up", has_above, above), ("down", has_below, below)):
                if way in ("own", direction) and hop + 1 < depth:
                    @pl.when(cond)
                    def _():
                        copy(held_at(core, chip, o, "ab"), ("z", direction, hop + 1), target).wait_send()
                        if rows_c:
                            copy(held_at(core, slice(None), o, "c"), ("zc", direction, hop + 1), target).wait_send()
        when(n, body)
    if rows_c:
        for name in ("cx", "cy", "cy2"):
            copy(held_at(core, chip, z, "c"), (name,), to_x).wait_send()


def semaphores(depth):
    return 13 * (2 * depth - 1) + 3


def fused(depth, columns, up_rows, mix_rows, ln_gain, mix_weight, mix_bias, out_weight):
    rows, channels = up_rows.shape
    groups = mix_weight.shape[0]
    shard_rows, shard_cols = out_weight.shape
    chips = columns // 2
    rows_c = shard_rows * 3 // 16 // 32 * 32
    any_space = pl.BlockSpec(memory_space=pl.ANY)
    vmem = pl.BlockSpec(memory_space=pltpu.VMEM)
    return pl.pallas_call(
        functools.partial(kernel, depth, rows_c),
        out_shape=pltpu.VMEM((rows, shard_cols * columns), jnp.bfloat16),
        in_specs=[any_space] * 6,
        out_specs=vmem,
        scratch_shapes=[
            pltpu.VMEM((2, chips, depth * shard_rows, shard_cols), jnp.bfloat16),
            pltpu.VMEM((1, channels), jnp.float32),
            pltpu.VMEM((groups, BLOCK), jnp.float32),
            pltpu.VMEM((rows, channels), jnp.bfloat16),
            pltpu.VMEM((rows, channels), jnp.bfloat16),
            pltpu.VMEM((groups, BLOCK, BLOCK), jnp.bfloat16),
            pltpu.VMEM((groups, BLOCK, BLOCK), jnp.bfloat16),
            pltpu.VMEM((groups, BLOCK, BLOCK), jnp.float32),
            pltpu.VMEM((BLOCK, channels), jnp.bfloat16),
            pltpu.VMEM((BLOCK, channels), jnp.bfloat16),
            pltpu.VMEM((rows, channels), jnp.bfloat16),
            pltpu.VMEM((rows, shard_cols * columns), jnp.float32),
            pltpu.SemaphoreType.DMA((4 + 2 * (rows // BLOCK),)),
            pltpu.SemaphoreType.DMA((semaphores(depth),)),
            pltpu.SemaphoreType.DMA((semaphores(depth),)),
        ],
        compiler_params=pltpu.CompilerParams(
            collective_id=0, has_side_effects=True, vmem_limit_bytes=60 * 2**20
        ),
    )(up_rows, mix_rows, ln_gain[None], mix_weight, mix_bias, out_weight)


def plain(up_rows, mix_rows, ln_gain, mix_weight, mix_bias, out_weight):
    up_act = gelu(up_rows.astype(jnp.float32)).astype(jnp.bfloat16)
    activated = gelu(mix_rows.astype(jnp.float32))
    center = jnp.mean(activated, axis=-1, keepdims=True)
    spread = jnp.mean(jnp.square(activated - center), axis=-1, keepdims=True)
    normed = ((activated - center) * lax.rsqrt(spread + norm_epsilon) * ln_gain).astype(
        jnp.bfloat16
    )
    positions = lax.broadcasted_iota(jnp.int32, (BLOCK, BLOCK), 0)
    sources = lax.broadcasted_iota(jnp.int32, (BLOCK, BLOCK), 1)
    masked = jnp.where((positions >= sources)[None], mix_weight, jnp.zeros_like(mix_weight))
    row_count, channels = normed.shape
    groups = masked.shape[0]
    blocks = normed.reshape(row_count // BLOCK, BLOCK, groups, channels // groups)
    mixed = jnp.einsum("gts,nsgc->ntgc", masked, blocks, preferred_element_type=jnp.float32)
    mixed = mixed + jnp.transpose(mix_bias)[None, :, :, None]
    gated = (up_act.astype(jnp.float32) * mixed.reshape(row_count, channels)).astype(jnp.bfloat16)
    rows_whole = lax.all_gather(out_weight, "sp", axis=0, tiled=True)
    whole = lax.all_gather(rows_whole, "dp", axis=1, tiled=True)
    return jnp.dot(gated, whole, preferred_element_type=jnp.float32).astype(jnp.bfloat16)


def solution(mesh):
    depth, columns = mesh.shape["sp"], mesh.shape["dp"]

    def per_device(up_pre, mix_pre, ln_gain, mix_weight, mix_bias, out_weight):
        shard_rows, shard_cols = out_weight.shape
        fits = (
            columns == 8
            and depth > 1
            and up_pre.shape[0] == 1
            and shard_cols % LANES == 0
            and shard_rows % LANES == 0
            and up_pre.shape[1] % BLOCK == 0
            and up_pre.shape[2] % (mix_weight.shape[0] * LANES) == 0
        )
        form = functools.partial(fused, depth, columns) if fits else plain
        return form(up_pre[0], mix_pre[0], ln_gain, mix_weight, mix_bias, out_weight)[None]

    return jax.shard_map(
        per_device,
        mesh=mesh,
        in_specs=(P("dp", "sp", None), P("dp", "sp", None), P(), P(), P(), P("sp", "dp")),
        out_specs=P("dp", "sp", None),
        check_vma=False,
    )
```
